32 devices in a mesh: ep: 8 (over z, y), tp: 4 (over x, core).
Axes of the slice: x: 2, y: 2, z: 4, core: 2. Of those that a mesh axis runs over, the one named last changes fastest.
Arguments:
- mixer_in: bfloat16 [4096, 4096], P(('ep', 'tp')), may hold values from -6 to 6
- mixer_gain: float32 [4096], replicated, may hold values from 0.1 to 1.9
- group_weight: bfloat16 [4, 1024, 1024], P('tp'), may hold values from -0.1875 to 0.1875
- group_scale: float32 [4, 1024], P('tp'), may hold values from 0.1 to 1.9
- expert_in: bfloat16 [4096, 4096], P(('ep', 'tp')), may hold values from -6 to 6
- expert_gain: float32 [4096], replicated, may hold values from 0.1 to 1.9
- routes: int32 [4096, 2], P('ep'), may hold values from 0 to 7, all different within a row; in each aligned block of 128 rows (0 to 127, 128 to 255, ...) at most 48 rows name the same one
- route_weight: float32 [4096, 2], P('ep'), may hold values from 0.2 to 1
- gate_weight: bfloat16 [8, 4096, 1024], P('ep', None, 'tp'), may hold values from -0.25 to 0.25
- up_weight: bfloat16 [8, 4096, 1024], P('ep', None, 'tp'), may hold values from -0.25 to 0.25
- down_weight: bfloat16 [8, 1024, 4096], P('ep', 'tp'), may hold values from -0.02734375 to 0.02734375
Outputs:
- mixed: bfloat16 [4096, 4096], P('ep', 'tp')
- expert_out: bfloat16 [4096, 4096], P(('ep', 'tp'))
The draws below stay inside these ranges and needn't reach their ends.
Inputs may be any that keep to these rules, and one draw needn't show every extreme that they name: `routes`: each row names 2 different experts; within the rows of one device (aligned blocks of 128 rows) no expert is named more than 48 times, and that count is reached.
All inputs are finite; a program needn't handle non-finite values.
Results may differ from the reference program's by a relative error of at most 0.012.
Values may be sent and summed in bfloat16 or wider, within the bound.
A program may use at most 128 MiB of HBM per device.

```python
import math
import jax
import jax.numpy as jnp
import numpy as np
from jax import lax

D = 4096
GROUPS = 4
GW = 1024
WMAX = 16
F = 1024
TOP = 2
TOK_B = 128
EXPERTS = 8
CAP = 48
TOKENS_A = 4096
TOKENS_B = 4096
N_TP = 4


def levels(rng, dims, cuts, low, high):
    loudness, own = 1.0, jax.random.fold_in(rng, 6)
    for axis_at, blocks in cuts:
        steps = jnp.exp(jax.random.uniform(jax.random.fold_in(own, axis_at), (blocks,), jnp.float32, low / len(cuts), high / len(cuts)))
        loudness = loudness * jnp.repeat(steps, dims[axis_at] // blocks).reshape([-1 if axis == axis_at else 1 for axis in range(len(dims))])
    return loudness


def assign_block(rng, own, number, rows, amount, top, bound, slope):
    ranking = jax.random.permutation(rng, amount)
    packed, ordinary = portions_of(amount, rows * top, bound, slope, True), portions_of(amount, rows * top, bound, slope, False)
    places = jnp.arange(amount)

    def named(tallies, offset_by):
        used = int((tallies > 0).sum())
        fixed = max(1, used // 4)
        shifted = fixed + (places - fixed + offset_by * (used - fixed)) % max(1, amount - fixed)
        return jnp.zeros((amount,), jnp.int32).at[ranking[jnp.where(places < fixed, places, shifted)]].set(jnp.asarray(tallies, jnp.int32))

    tallies = jnp.where(number % 4 == 0, named(packed, number // 4), named(ordinary, number - number // 4 - 1))
    mixed = jax.random.permutation(jax.random.fold_in(own, 3), amount)
    source_of, receiver = mixed[0:amount // 2 * 2:2], mixed[1:amount // 2 * 2:2]
    slack = jnp.minimum(tallies[source_of] - 1, bound - tallies[receiver]) // 2
    slack = jnp.where((source_of == ranking[0]) | (receiver == ranking[0]) | (tallies[receiver] == 0), 0, jnp.maximum(slack, 0))
    shifted = jax.random.randint(jax.random.fold_in(own, 4), (amount // 2,), 0, 1 << 20) % (slack + 1)
    tallies = tallies.at[source_of].add(-shifted).at[receiver].add(shifted)
    members = jnp.searchsorted(jnp.cumsum(tallies), jnp.arange(rows * top), side="right").astype(jnp.int32)
    listing = members.reshape(top, rows).T
    listing = listing[jax.random.permutation(jax.random.fold_in(own, 1), rows)]
    offset_by = jax.random.randint(jax.random.fold_in(own, 2), (rows, 1), 0, top)
    return jnp.take_along_axis(listing, (jnp.arange(top)[None, :] + offset_by) % top, axis=1)


def portions_of(amount, total, bound, skew, full):
    portions = [(1 << 20) // math.isqrt(rank ** skew) + 1 for rank in range(1, amount + 1)]
    largest = bound if full else min(bound, max(-(-total // amount), total * portions[0] // sum(portions)))
    least = 1 if total - largest >= amount - 1 else 0
    given, surplus = [largest] + [least] * (amount - 1), total - largest - least * (amount - 1)
    while surplus > 0:
        movable = [i for i in range(1, amount) if given[i] < largest] or [i for i in range(1, amount) if given[i] < bound]
        mass, budget = sum([portions[i] for i in movable]), surplus
        for i in movable:
            more = min(bound - given[i], max(1, budget * portions[i] // mass), surplus)
            given[i] = given[i] + more
            surplus = surplus - more
    return np.array(given)


def bell_draw(own_key, extent, width, bound, cuts=(), kind=jnp.bfloat16):
    result = width * jax.random.normal(own_key, extent, jnp.float32)
    if cuts:
        result = result * levels(own_key, extent, cuts, -0.22, 0.18)
    return jnp.clip(result, -bound, bound).astype(kind)


def setup_inputs(seed: int = 0) -> dict:
    key_of = jax.random.split(jax.random.key(seed), 12)
    mixer_in = bell_draw(key_of[0], (TOKENS_A, D), 1.0, 6.0, ((0, 32),))
    mixer_gain = jnp.clip(1.0 + 0.18 * jax.random.normal(key_of[1], (D,), jnp.float32), 0.1, 1.9)
    group_weight = bell_draw(key_of[2], (GROUPS, GW, GW), GW ** -0.5, 0.1875, ((0, 4),))
    group_scale = jnp.clip(1.0 + 0.18 * jax.random.normal(key_of[3], (GROUPS, GW), jnp.float32), 0.1, 1.9)
    expert_in = bell_draw(key_of[4], (TOKENS_B, D), 1.0, 6.0, ((0, 32),))
    expert_gain = jnp.clip(1.0 + 0.18 * jax.random.normal(key_of[5], (D,), jnp.float32), 0.1, 1.9)
    routes_keys = jax.random.split(jax.random.fold_in(key_of[6], 1), TOKENS_B // TOK_B)
    routes_turns = jax.random.permutation(jax.random.fold_in(key_of[6], 3), TOKENS_B // TOK_B)
    routes = jax.vmap(lambda own, number: assign_block(jax.random.fold_in(key_of[6], 2), own, number, TOK_B, EXPERTS, TOP, CAP, 2))(routes_keys, routes_turns).reshape((TOKENS_B, TOP))
    route_weight = jnp.clip(0.2 + 0.8 * jax.random.uniform(key_of[7], (TOKENS_B, TOP), jnp.float32) ** levels(key_of[7], (TOKENS_B, TOP), ((0, 8),), -0.2, 0.2), 0.2, 1.0)
    gate_weight = bell_draw(key_of[8], (EXPERTS, D, F), (D // 9) ** -0.5, 0.25, ((0, 8), (2, 4)))
    up_weight = bell_draw(key_of[9], (EXPERTS, D, F), (D // 9) ** -0.5, 0.25, ((0, 8), (2, 4)))
    down_weight = bell_draw(key_of[10], (EXPERTS, F, D), (45 * F) ** -0.5, 0.02734375, ((0, 8), (1, 4)))
    return {"mixer_in": mixer_in, "mixer_gain": mixer_gain, "group_weight": group_weight, "group_scale": group_scale, "expert_in": expert_in, "expert_gain": expert_gain, "routes": routes, "route_weight": route_weight, "gate_weight": gate_weight, "up_weight": up_weight, "down_weight": down_weight}


epsilon = 1e-06
clamp_limit = 7.0
sigmoid_slope = 1.702

def rms_norm(values, gain):
    widened = values.astype(jnp.float32)
    scaled = widened * lax.rsqrt(lax.optimization_barrier(jnp.mean(widened * widened, axis=-1, keepdims=True)) + epsilon)
    return (scaled * gain).astype(jnp.bfloat16)

def clamped_unit(gate_part, up_part):
    gate_part = jnp.minimum(gate_part, clamp_limit)
    up_part = jnp.clip(up_part, -clamp_limit, clamp_limit)
    return ((up_part + 1.0) * gate_part * jax.nn.sigmoid(sigmoid_slope * gate_part)).astype(jnp.bfloat16)

def slot_table(block_routes, experts, capacity):
    count = block_routes.shape[0]
    onehot = (block_routes[:, :, None] == jnp.arange(experts, dtype=jnp.int32)[None, None, :]).astype(jnp.int32)
    per_token = lax.optimization_barrier(jnp.sum(onehot, axis=1))
    earlier = jnp.cumsum(per_token, axis=0) - per_token
    slot_rank = lax.optimization_barrier(jnp.sum(onehot * earlier[:, None, :], axis=2))
    matches = onehot[:, :, :, None] * (slot_rank[:, :, None, None] == jnp.arange(capacity, dtype=jnp.int32)[None, None, None, :]).astype(jnp.int32)
    source = lax.optimization_barrier(jnp.sum(matches * jnp.arange(count, dtype=jnp.int32)[:, None, None, None], axis=(0, 1)))
    filled = lax.optimization_barrier(jnp.sum(matches, axis=(0, 1)))
    return (source, filled, slot_rank)

def reference(mixer_in, mixer_gain, group_weight, group_scale, expert_in, expert_gain, routes, route_weight, gate_weight, up_weight, down_weight):
    normed = rms_norm(mixer_in, mixer_gain)
    length = normed.shape[0]
    position = jnp.arange(length, dtype=jnp.int32)
    pieces = []
    for group in range(GROUPS):
        window = 2 ** (group + 1)
        values = normed[:, group * GW:(group + 1) * GW].astype(jnp.float32)
        padded = jnp.pad(values, ((WMAX - 1, 0), (0, 0)))
        window_sum = jnp.zeros_like(values)
        for offset in range(window):
            window_sum = window_sum + padded[WMAX - 1 - offset:WMAX - 1 - offset + length]
        counts = jnp.minimum(position + 1, window).astype(jnp.float32)[:, None]
        pooled = (window_sum / counts - values).astype(jnp.bfloat16)
        product = jnp.dot(pooled, group_weight[group], preferred_element_type=jnp.float32)
        pieces.append((product * group_scale[group]).astype(jnp.bfloat16))
    mixed = jnp.concatenate(pieces, axis=1)
    expert_norm = rms_norm(expert_in, expert_gain)
    blocks = expert_norm.shape[0] // TOK_B
    block_routes = routes.reshape(blocks, TOK_B, TOP)
    source, filled, slot_rank = lax.map(lambda item: slot_table(item, EXPERTS, CAP), block_routes)
    global_index = source + (jnp.arange(blocks, dtype=jnp.int32) * TOK_B)[:, None, None]
    part_width = F // N_TP

    def one_expert(expert):
        slot_index = lax.dynamic_index_in_dim(global_index, expert, 1, keepdims=False).reshape(-1)
        present = lax.dynamic_index_in_dim(filled, expert, 1, keepdims=False).reshape(-1)
        picked = expert_norm[slot_index] * present[:, None].astype(jnp.bfloat16)
        gate_part = jnp.dot(picked, gate_weight[expert], preferred_element_type=jnp.float32)
        up_part = jnp.dot(picked, up_weight[expert], preferred_element_type=jnp.float32)
        hidden = clamped_unit(gate_part, up_part)
        total = jnp.zeros((picked.shape[0], picked.shape[1]), jnp.float32)
        for part in range(N_TP):
            partial_value = jnp.dot(hidden[:, part * part_width:(part + 1) * part_width], down_weight[expert][part * part_width:(part + 1) * part_width], preferred_element_type=jnp.float32).astype(jnp.bfloat16)
            total = total + lax.optimization_barrier(partial_value).astype(jnp.float32)
        return total.astype(jnp.bfloat16).reshape(blocks, CAP, picked.shape[1])
    results = lax.map(one_expert, jnp.arange(EXPERTS, dtype=jnp.int32))
    flat_rows = results.reshape(-1, results.shape[-1])
    block_of = (jnp.arange(expert_norm.shape[0], dtype=jnp.int32) // TOK_B)[:, None]
    slot_index = (routes * blocks + block_of) * CAP + slot_rank.reshape(-1, TOP)
    expert_sum = jnp.zeros(expert_norm.shape, jnp.float32)
    for choice_slot in range(TOP):
        expert_sum = expert_sum + flat_rows[slot_index[:, choice_slot]].astype(jnp.float32) * route_weight[:, choice_slot:choice_slot + 1]
    return (mixed, expert_sum.astype(jnp.bfloat16))
```

```python
import jax
import jax.numpy as jnp
from jax import lax
from jax.sharding import PartitionSpec as P

WMAX = 16
CHUNKS = 3

epsilon = 1e-06
clamp_limit = 7.0
sigmoid_slope = 1.702


def from_behind(x, axis, by):
    count = lax.axis_size(axis)
    pairs = [(i, i + by) for i in range(count) if 0 <= i + by < count]
    return lax.ppermute(x, axis, pairs)


def rms_norm(values, gain):
    widened = values.astype(jnp.float32)
    scaled = widened * lax.rsqrt(jnp.mean(widened * widened, axis=-1, keepdims=True) + epsilon)
    return (scaled * gain).astype(jnp.bfloat16)


def clamped_unit(gate_part, up_part):
    gate_part = jnp.minimum(gate_part, clamp_limit)
    up_part = jnp.clip(up_part, -clamp_limit, clamp_limit)
    return ((up_part + 1.0) * gate_part * jax.nn.sigmoid(sigmoid_slope * gate_part)).astype(
        jnp.bfloat16
    )


def slot_ids(block_routes, experts, capacity):
    onehot = (
        block_routes[:, :, None] == jnp.arange(experts, dtype=jnp.int32)[None, None, :]
    ).astype(jnp.float32)
    per_token = jnp.sum(onehot, axis=1)
    count = block_routes.shape[0]
    before = (
        jnp.arange(count, dtype=jnp.int32)[:, None] > jnp.arange(count, dtype=jnp.int32)[None, :]
    ).astype(jnp.bfloat16)
    earlier = jnp.dot(before, per_token.astype(jnp.bfloat16), preferred_element_type=jnp.float32)
    rank = jnp.sum(onehot * earlier[:, None, :], axis=2).astype(jnp.int32)
    return block_routes, rank


def mixer(mixer_in, mixer_gain, group_weight, group_scale):
    normed = rms_norm(mixer_in, mixer_gain)
    shard_rows = lax.all_to_all(normed, "tp", split_axis=1, concat_axis=0, tiled=True)
    length = shard_rows.shape[0]
    before = from_behind(shard_rows[length - WMAX :], "ep", 1)
    total = jnp.concatenate([before, shard_rows], axis=0).astype(jnp.float32)
    values = total[WMAX:]
    tp_index = lax.axis_index("tp")
    window = 2 << tp_index
    position = lax.axis_index("ep") * length + jnp.arange(length, dtype=jnp.int32)
    picked = jnp.zeros_like(values)
    reach = 1
    for level in range(lax.axis_size("tp")):
        total = total[reach:] + total[:-reach]
        reach = 2 * reach
        picked = jnp.where(tp_index == level, total[total.shape[0] - length :], picked)
    counts = jnp.minimum(position + 1, window).astype(jnp.float32)[:, None]
    pooled = (picked / counts - values).astype(jnp.bfloat16)
    return (
        jnp.dot(pooled, group_weight[0], preferred_element_type=jnp.float32) * group_scale[0]
    ).astype(jnp.bfloat16)


def shards(
    mixer_in,
    mixer_gain,
    group_weight,
    group_scale,
    expert_in,
    expert_gain,
    routes,
    route_weight,
    gate_weight,
    up_weight,
    down_weight,
):
    mixed = mixer(mixer_in, mixer_gain, group_weight, group_scale)
    expert_norm = rms_norm(expert_in, expert_gain)
    tok_count, width = expert_in.shape
    top = routes.shape[1]
    experts = lax.axis_size("ep")
    capacity = max(2, 3 * tok_count * top // (2 * experts))
    chunks = CHUNKS if capacity % CHUNKS == 0 else 1
    part = capacity // chunks
    tp_index = lax.axis_index("tp")
    own_routes = lax.dynamic_slice_in_dim(routes, tp_index * tok_count, tok_count, 0)
    own_weight = lax.dynamic_slice_in_dim(route_weight, tp_index * tok_count, tok_count, 0)
    gate_local = gate_weight[0]
    up_local = up_weight[0]
    down_full = lax.all_gather(down_weight[0], "tp", axis=0, tiled=True)
    expert_of, rank = slot_ids(own_routes, experts, capacity)
    expert_sum = jnp.zeros((tok_count, width), jnp.float32)
    pieces = []
    picks = []
    for chunk in range(chunks):
        inside = (rank >= chunk * part) & (rank < (chunk + 1) * part)
        slot = jnp.where(inside, expert_of * part + rank - chunk * part, -1)
        match = slot[:, :, None] == jnp.arange(experts * part, dtype=jnp.int32)[None, None, :]
        picks.append(match)
        pick = jnp.any(match, axis=1).astype(jnp.bfloat16)
        outgoing = lax.dot_general(
            pick, expert_norm, (((0,), (0,)), ((), ())), preferred_element_type=jnp.float32
        ).astype(jnp.bfloat16)
        arrived = lax.all_to_all(outgoing, "ep", split_axis=0, concat_axis=0, tiled=True)
        pieces.append(lax.all_gather(arrived, "tp", axis=0, tiled=True))
    for chunk in range(chunks):
        piece = pieces[chunk]
        hidden = clamped_unit(
            jnp.dot(piece, gate_local, preferred_element_type=jnp.float32),
            jnp.dot(piece, up_local, preferred_element_type=jnp.float32),
        )
        hidden = lax.all_to_all(hidden, "tp", split_axis=0, concat_axis=1, tiled=True)
        result = jnp.dot(hidden, down_full, preferred_element_type=jnp.float32).astype(jnp.bfloat16)
        returned = lax.all_to_all(result, "ep", split_axis=0, concat_axis=0, tiled=True)
        weights = jnp.sum(jnp.where(picks[chunk], own_weight[:, :, None], 0.0), axis=1)
        high = weights.astype(jnp.bfloat16)
        low = (weights - high.astype(jnp.float32)).astype(jnp.bfloat16)
        expert_sum = (
            expert_sum
            + jnp.dot(high, returned, preferred_element_type=jnp.float32)
            + jnp.dot(low, returned, preferred_element_type=jnp.float32)
        )
    return (mixed, expert_sum.astype(jnp.bfloat16))


def solution(mesh):
    in_specs = (
        P(("ep", "tp"), None),
        P(),
        P("tp", None, None),
        P("tp", None),
        P(("ep", "tp"), None),
        P(),
        P("ep", None),
        P("ep", None),
        P("ep", None, "tp"),
        P("ep", None, "tp"),
        P("ep", "tp", None),
    )
    out_specs = (P("ep", "tp"), P(("ep", "tp"), None))
    return jax.shard_map(shards, mesh=mesh, in_specs=in_specs, out_specs=out_specs, check_vma=False)
```

```python
import jax
import jax.numpy as jnp
from jax import lax
from jax.sharding import PartitionSpec as P

WMAX = 16
CHUNKS = 3

epsilon = 1e-06
clamp_limit = 7.0
sigmoid_slope = 1.702


def from_behind(x, axis, by):
    count = lax.axis_size(axis)
    pairs = [(i, i + by) for i in range(count) if 0 <= i + by < count]
    return lax.ppermute(x, axis, pairs)


def rms_norm(values, gain):
    widened = values.astype(jnp.float32)
    scaled = widened * lax.rsqrt(jnp.mean(widened * widened, axis=-1, keepdims=True) + epsilon)
    return (scaled * gain).astype(jnp.bfloat16)


def clamped_unit(gate_part, up_part):
    gate_part = jnp.minimum(gate_part, clamp_limit)
    up_part = jnp.clip(up_part, -clamp_limit, clamp_limit)
    return ((up_part + 1.0) * gate_part * jax.nn.sigmoid(sigmoid_slope * gate_part)).astype(
        jnp.bfloat16
    )


def slot_ids(block_routes, experts, capacity):
    onehot = (
        block_routes[:, :, None] == jnp.arange(experts, dtype=jnp.int32)[None, None, :]
    ).astype(jnp.float32)
    per_token = jnp.sum(onehot, axis=1)
    count = block_routes.shape[0]
    before = (
        jnp.arange(count, dtype=jnp.int32)[:, None] > jnp.arange(count, dtype=jnp.int32)[None, :]
    ).astype(jnp.bfloat16)
    earlier = jnp.dot(before, per_token.astype(jnp.bfloat16), preferred_element_type=jnp.float32)
    rank = jnp.sum(onehot * earlier[:, None, :], axis=2).astype(jnp.int32)
    return block_routes, rank


def mixer_rows(mixer_in, mixer_gain):
    normed = rms_norm(mixer_in, mixer_gain)
    shard_rows = lax.all_to_all(normed, "tp", split_axis=1, concat_axis=0, tiled=True)
    length = shard_rows.shape[0]
    return shard_rows, from_behind(shard_rows[length - WMAX :], "ep", 1)


def mixer(shard_rows, before, group_weight, group_scale):
    length = shard_rows.shape[0]
    total = jnp.concatenate([before, shard_rows], axis=0).astype(jnp.float32)
    values = total[WMAX:]
    tp_index = lax.axis_index("tp")
    window = 2 << tp_index
    position = lax.axis_index("ep") * length + jnp.arange(length, dtype=jnp.int32)
    picked = jnp.zeros_like(values)
    reach = 1
    for level in range(lax.axis_size("tp")):
        total = total[reach:] + total[:-reach]
        reach = 2 * reach
        picked = jnp.where(tp_index == level, total[total.shape[0] - length :], picked)
    counts = jnp.minimum(position + 1, window).astype(jnp.float32)[:, None]
    pooled = (picked / counts - values).astype(jnp.bfloat16)
    return (
        jnp.dot(pooled, group_weight[0], preferred_element_type=jnp.float32) * group_scale[0]
    ).astype(jnp.bfloat16)


def shards(
    mixer_in,
    mixer_gain,
    group_weight,
    group_scale,
    expert_in,
    expert_gain,
    routes,
    route_weight,
    gate_weight,
    up_weight,
    down_weight,
):
    shard_rows, before = mixer_rows(mixer_in, mixer_gain)
    expert_in, shard_rows, before = lax.optimization_barrier((expert_in, shard_rows, before))
    mixed = mixer(shard_rows, before, group_weight, group_scale)
    expert_norm = rms_norm(expert_in, expert_gain)
    tok_count, width = expert_in.shape
    top = routes.shape[1]
    experts = lax.axis_size("ep")
    capacity = max(2, 3 * tok_count * top // (2 * experts))
    chunks = CHUNKS if capacity % CHUNKS == 0 else 1
    part = capacity // chunks
    tp_index = lax.axis_index("tp")
    own_routes = lax.dynamic_slice_in_dim(routes, tp_index * tok_count, tok_count, 0)
    own_weight = lax.dynamic_slice_in_dim(route_weight, tp_index * tok_count, tok_count, 0)
    gate_local = gate_weight[0]
    up_local = up_weight[0]
    down_full = lax.all_gather(down_weight[0], "tp", axis=0, tiled=True)
    expert_of, rank = slot_ids(own_routes, experts, capacity)
    expert_sum = jnp.zeros((tok_count, width), jnp.float32)
    pieces = []
    picks = []
    for chunk in range(chunks):
        inside = (rank >= chunk * part) & (rank < (chunk + 1) * part)
        slot = jnp.where(inside, expert_of * part + rank - chunk * part, -1)
        match = slot[:, :, None] == jnp.arange(experts * part, dtype=jnp.int32)[None, None, :]
        picks.append(match)
        pick = jnp.any(match, axis=1).astype(jnp.bfloat16)
        outgoing = lax.dot_general(
            pick, expert_norm, (((0,), (0,)), ((), ())), preferred_element_type=jnp.float32
        ).astype(jnp.bfloat16)
        if chunk > 0:
            outgoing, arrived = lax.optimization_barrier((outgoing, arrived))
        arrived = lax.all_to_all(outgoing, "ep", split_axis=0, concat_axis=0, tiled=True)
        if chunk == 1:
            arrived, down_full = lax.optimization_barrier((arrived, down_full))
        pieces.append(lax.all_gather(arrived, "tp", axis=0, tiled=True))
    for chunk in range(chunks):
        piece = pieces[chunk]
        if chunk > 0:
            piece, result = lax.optimization_barrier((piece, result))
        hidden = clamped_unit(
            jnp.dot(piece, gate_local, preferred_element_type=jnp.float32),
            jnp.dot(piece, up_local, preferred_element_type=jnp.float32),
        )
        hidden = lax.all_to_all(hidden, "tp", split_axis=0, concat_axis=1, tiled=True)
        result = jnp.dot(hidden, down_full, preferred_element_type=jnp.float32).astype(jnp.bfloat16)
        returned = lax.all_to_all(result, "ep", split_axis=0, concat_axis=0, tiled=True)
        weights = jnp.sum(jnp.where(picks[chunk], own_weight[:, :, None], 0.0), axis=1)
        high = weights.astype(jnp.bfloat16)
        low = (weights - high.astype(jnp.float32)).astype(jnp.bfloat16)
        expert_sum = (
            expert_sum
            + jnp.dot(high, returned, preferred_element_type=jnp.float32)
            + jnp.dot(low, returned, preferred_element_type=jnp.float32)
        )
    return (mixed, expert_sum.astype(jnp.bfloat16))


def solution(mesh):
    in_specs = (
        P(("ep", "tp"), None),
        P(),
        P("tp", None, None),
        P("tp", None),
        P(("ep", "tp"), None),
        P(),
        P("ep", None),
        P("ep", None),
        P("ep", None, "tp"),
        P("ep", None, "tp"),
        P("ep", "tp", None),
    )
    out_specs = (P("ep", "tp"), P(("ep", "tp"), None))
    return jax.shard_map(shards, mesh=mesh, in_specs=in_specs, out_specs=out_specs, check_vma=False)
```
